32 devices in a mesh: sp: 16 (over z, y, x), tp: 2 (over core).
Axes of the slice: x: 2, y: 2, z: 4, core: 2. Of those that a mesh axis runs over, the one named last changes fastest.
Arguments:
- resid: bfloat16 [6144, 2048], P('sp'), may hold values from -6 to 6
- x_branch: bfloat16 [6144, 2048], P('sp', 'tp'), may hold values from -6 to 6
- gate_branch: bfloat16 [6144, 2048], P('sp', 'tp'), may hold values from -6 to 6
- conv_w: float32 [4, 2048], P(None, 'tp'), may hold values from -3 to 3
- gate_a_w: bfloat16 [32, 64, 64], P('tp'), may hold values from -0.75 to 0.75
- gate_x_w: bfloat16 [32, 64, 64], P('tp'), may hold values from -0.75 to 0.75
- decay_rate: float32 [2048], P('tp'), may hold values from 0 to 0.01, as said below
- decay_extra: float32 [6144, 2048], P('sp', 'tp'), may hold values from -3 to 0, as said below
- w_proj: bfloat16 [2048, 2048], P('tp'), may hold values from -0.125 to 0.125
- mix_gain: float32 [2048], replicated, may hold values from 0.1 to 1.9
- pre_gain: float32 [2048], replicated, may hold values from 0.1 to 1.9
- w_gate: bfloat16 [2048, 5632], P('sp', 'tp'), may hold values from -0.125 to 0.125
- w_up: bfloat16 [2048, 5632], P('sp', 'tp'), may hold values from -0.125 to 0.125
- w_down: bfloat16 [5632, 2048], P('tp', 'sp'), may hold values from -0.078125 to 0.078125
- out_gain: float32 [2048], replicated, may hold values from 0.1 to 1.9
Outputs:
- stream_out: bfloat16 [6144, 2048], P(('sp', 'tp'))
The draws below stay inside these ranges and needn't reach their ends.
Inputs may be any that keep to these rules, and one draw needn't show every extreme that they name: `decay_rate`: positive rates. `decay_extra`: non-positive values.
All inputs are finite; a program needn't handle non-finite values.
Results may differ from the reference program's by a relative error of at most 0.015.
Values may be sent and summed in bfloat16 or wider, within the bound.
A program may use at most 128 MiB of HBM per device.

```python
import math
import jax
import jax.numpy as jnp
from jax import lax

D = 2048
BLOCKS = 32
BW = 64
RECURRENCE_WIDTH = 2048
FF = 5632
CONV = 4
TOK_DEV = 384
TOKEN_SLOTS = 6144
N_TP = 2


def draw_decay_rate(key, part):
    key_pick, key_fast, key_slow = jax.random.split(key, 3)
    fast_share = 0.5
    is_fast = jax.random.uniform(key_pick, (RECURRENCE_WIDTH,), jnp.float32) < fast_share
    fast_rate = jnp.exp(jax.random.uniform(key_fast, (RECURRENCE_WIDTH,), jnp.float32, minval=math.log(1.0 / 240.0), maxval=math.log(1.0 / 120.0)))
    slow_rate = math.log(10.0) / (16.0 * TOKEN_SLOTS) * jax.random.uniform(key_slow, (RECURRENCE_WIDTH,), jnp.float32, minval=0.25, maxval=1.0)
    return jnp.where(is_fast, fast_rate, slow_rate).astype(jnp.float32)


def draw_decay_extra(key, part):
    key_level, key_location_draw, key_extent_draw = jax.random.split(key, 3)
    nblocks = TOKEN_SLOTS // TOK_DEV
    levels = jax.random.uniform(key_level, (nblocks, RECURRENCE_WIDTH), jnp.float32) * (-0.5 / TOKEN_SLOTS)
    drawn_regime = jnp.repeat(levels, TOK_DEV, axis=0)
    spike_token_rows = jax.random.randint(key_location_draw, (3,), 0, TOKEN_SLOTS)
    spike_extent = jax.random.uniform(key_extent_draw, (3, RECURRENCE_WIDTH), jnp.float32, minval=math.log(0.5), maxval=math.log(0.8))
    token_offsets = jnp.arange(TOKEN_SLOTS)
    inside_spike = (token_offsets[:, None] == spike_token_rows[None, :]).astype(jnp.float32)
    return (drawn_regime + jnp.dot(inside_spike, spike_extent)).astype(jnp.float32)


def block_scale(own_key, extent, cuts, least, largest):
    factor_of = 1.0
    for axis_at, parts in cuts:
        steps = jax.random.uniform(jax.random.fold_in(jax.random.fold_in(own_key, 6), axis_at), (parts,), jnp.float32, least / len(cuts), largest / len(cuts))
        factor_of = factor_of * jnp.repeat(jnp.exp(steps), extent[axis_at] // parts).reshape((-1,) + (1,) * (len(extent) - 1 - axis_at))
    return factor_of


def bell_draw(key, dims, width, reach, shards=(), held_as=jnp.bfloat16):
    array = width * jax.random.normal(key, dims, jnp.float32)
    if shards:
        array = array * block_scale(key, dims, shards, -0.22, 0.18)
    return jnp.clip(array, -reach, reach).astype(held_as)


def setup_inputs(seed: int = 0) -> dict:
    seeds = jax.random.split(jax.random.key(seed), 16)
    return {
        "resid": bell_draw(seeds[0], (TOKEN_SLOTS, D), 1.0, 6.0, ((0, 16),)),
        "x_branch": bell_draw(seeds[1], (TOKEN_SLOTS, RECURRENCE_WIDTH), 1.0, 6.0, ((0, 16), (1, 2))),
        "gate_branch": bell_draw(seeds[2], (TOKEN_SLOTS, RECURRENCE_WIDTH), 1.0, 6.0, ((0, 16), (1, 2))),
        "conv_w": bell_draw(seeds[3], (CONV, RECURRENCE_WIDTH), CONV ** -0.5, 3.0, ((1, 2),), jnp.float32),
        "gate_a_w": bell_draw(seeds[4], (BLOCKS, BW, BW), BW ** -0.5, 0.75, ((0, 2),)),
        "gate_x_w": bell_draw(seeds[5], (BLOCKS, BW, BW), BW ** -0.5, 0.75, ((0, 2),)),
        "decay_rate": draw_decay_rate(jax.random.fold_in(seeds[15], 71), 0),
        "decay_extra": draw_decay_extra(jax.random.fold_in(seeds[15], 71), 0),
        "w_proj": bell_draw(seeds[8], (RECURRENCE_WIDTH, D), RECURRENCE_WIDTH ** -0.5, 0.125, ((0, 2),)),
        "mix_gain": jnp.clip(1.0 + 0.18 * jax.random.normal(seeds[9], (D,), jnp.float32), 0.1, 1.9),
        "pre_gain": jnp.clip(1.0 + 0.18 * jax.random.normal(seeds[10], (D,), jnp.float32), 0.1, 1.9),
        "w_gate": bell_draw(seeds[11], (D, FF), D ** -0.5, 0.125, ((0, 16), (1, 2))),
        "w_up": bell_draw(seeds[12], (D, FF), D ** -0.5, 0.125, ((0, 16), (1, 2))),
        "w_down": bell_draw(seeds[13], (FF, D), FF ** -0.5, 0.078125, ((0, 2), (1, 16))),
        "out_gain": jnp.clip(1.0 + 0.18 * jax.random.normal(seeds[14], (D,), jnp.float32), 0.1, 1.9),
    }


LRU_SCALE = 8.0
NORM_EPS = 1e-06

def chain(earlier, later):
    return (earlier[0] * later[0], later[0] * earlier[1] + later[1])

def rms_scale(values, gains):
    return values * lax.rsqrt(lax.optimization_barrier(jnp.mean(values * values, axis=-1, keepdims=True)) + NORM_EPS) * gains

def reference(resid, x_branch, gate_branch, conv_w, gate_a_w, gate_x_w, decay_rate, decay_extra, w_proj, mix_gain, pre_gain, w_gate, w_up, w_down, out_gain):
    padded = jnp.pad(x_branch.astype(jnp.float32), ((CONV - 1, 0), (0, 0)))
    conv = padded[0:TOKEN_SLOTS] * conv_w[0]
    for tap in range(1, CONV):
        conv = conv + padded[tap:tap + TOKEN_SLOTS] * conv_w[tap]
    conv_out = conv.astype(jnp.bfloat16)
    grouped = conv_out.astype(jnp.float32).reshape(TOKEN_SLOTS, BLOCKS, BW)
    recur = jax.nn.sigmoid(jnp.einsum('rnc,ncd->rnd', grouped, gate_a_w.astype(jnp.float32)).reshape(TOKEN_SLOTS, RECURRENCE_WIDTH))
    inject = jax.nn.sigmoid(jnp.einsum('rnc,ncd->rnd', grouped, gate_x_w.astype(jnp.float32)).reshape(TOKEN_SLOTS, RECURRENCE_WIDTH))
    log_decay = -LRU_SCALE * recur * decay_rate + decay_extra
    decay = jnp.exp(log_decay)
    drive = jnp.sqrt(-jnp.expm1(2.0 * log_decay)) * inject * conv_out.astype(jnp.float32)
    _, state = lax.associative_scan(chain, (decay, drive), axis=0)
    mixer = (state * jax.nn.gelu(gate_branch.astype(jnp.float32))).astype(jnp.bfloat16)
    group_w = RECURRENCE_WIDTH // N_TP
    mixed = jnp.zeros((TOKEN_SLOTS, D), jnp.float32)
    for group in range(N_TP):
        partial_sum = jnp.dot(mixer[:, group * group_w:(group + 1) * group_w], w_proj[group * group_w:(group + 1) * group_w], preferred_element_type=jnp.float32)
        mixed = mixed + lax.optimization_barrier(partial_sum.astype(jnp.bfloat16)).astype(jnp.float32)
    stream = resid.astype(jnp.float32) + rms_scale(mixed, mix_gain)
    normed = rms_scale(stream, pre_gain).astype(jnp.bfloat16)
    group_f = FF // N_TP
    ffn = jnp.zeros((TOKEN_SLOTS, D), jnp.float32)
    for group in range(N_TP):
        gate = jnp.dot(normed, w_gate[:, group * group_f:(group + 1) * group_f], preferred_element_type=jnp.float32)
        upward = jnp.dot(normed, w_up[:, group * group_f:(group + 1) * group_f], preferred_element_type=jnp.float32)
        hidden = (jax.nn.silu(gate) * upward).astype(jnp.bfloat16)
        partial_sum = jnp.dot(hidden, w_down[group * group_f:(group + 1) * group_f], preferred_element_type=jnp.float32)
        ffn = ffn + lax.optimization_barrier(partial_sum.astype(jnp.bfloat16)).astype(jnp.float32)
    return (stream + 0.5 * rms_scale(ffn, out_gain)).astype(jnp.bfloat16)
```

```python
import functools

import jax
import jax.numpy as jnp
from jax import lax
from jax.experimental import pallas as pl
from jax.experimental.pallas import tpu as pltpu
from jax.sharding import PartitionSpec as P

LRU_SCALE = 8.0
NORM_EPS = 1e-06
LANES = 128
SEGMENTS = 8
HALO = 16
MESH = pl.DeviceIdType.MESH


def neg_expm1(u):
    near = 1.0 + u * (1.0 / 8.0)
    for k in range(7, 1, -1):
        near = 1.0 + (u * (1.0 / k)) * near
    return jnp.where(u > -0.35, -u * near, 1.0 - jnp.exp(u))


def mixer_kernel(
    n,
    taps,
    x_ref,
    gate_ref,
    conv_ref,
    ga_ref,
    gx_ref,
    rate_ref,
    extra_ref,
    out_ref,
    halo,
    padded,
    decay,
    drive,
    seg_p,
    seg_h,
    mine,
    slots,
    halo_send,
    halo_recv,
    send_sems,
    recv_sems,
):
    me = lax.axis_index("sp")
    length, width = x_ref.shape
    blocks = width // LANES
    span = length // SEGMENTS

    barrier = pltpu.get_barrier_semaphore()

    def greet(k, carry):
        pl.semaphore_signal(
            barrier, inc=1, device_id={"sp": lax.rem(me + k, n)}, device_id_type=MESH
        )
        return carry

    lax.fori_loop(1, n, greet, 0)
    pl.semaphore_wait(barrier, n - 1)

    tail = pltpu.make_async_remote_copy(
        src_ref=x_ref.at[pl.ds(length - HALO, HALO)],
        dst_ref=halo,
        send_sem=halo_send,
        recv_sem=halo_recv,
        device_id={"sp": lax.rem(me + 1, n)},
        device_id_type=MESH,
    )
    tail.start()
    tail.wait()

    first_place = (me > 0).astype(jnp.float32)

    def one_block(c, carry):
        cols = pl.ds(pl.multiple_of(c * LANES, LANES), LANES)
        padded[pl.ds(8, length), :] = x_ref[:, cols].astype(jnp.float32)
        padded[pl.ds(0, 8), :] = halo[pl.ds(HALO - 8, 8), cols].astype(jnp.float32) * first_place
        start = 8 - (taps - 1)
        conv = padded[pl.ds(start, length), :] * conv_ref[pl.ds(0, 1), cols]
        for tap in range(1, taps):
            conv = conv + padded[pl.ds(start + tap, length), :] * conv_ref[pl.ds(tap, 1), cols]
        conv_out = conv.astype(jnp.bfloat16)
        recur = jax.nn.sigmoid(
            jnp.dot(conv_out, ga_ref[c], preferred_element_type=jnp.float32)
        )
        inject = jax.nn.sigmoid(
            jnp.dot(conv_out, gx_ref[c], preferred_element_type=jnp.float32)
        )
        log_decay = -LRU_SCALE * recur * rate_ref[pl.ds(0, 1), cols] + extra_ref[:, cols]
        decay[c] = jnp.exp(log_decay)
        room = neg_expm1(2.0 * log_decay)
        root = jnp.where(room > 0.0, jnp.sqrt(jnp.maximum(room, 1e-37)), 0.0)
        drive[c] = root * inject * conv_out.astype(jnp.float32)
        return carry

    lax.fori_loop(0, blocks, one_block, 0)

    def step(j, carry):
        prods, states = carry
        new_p, new_h = [], []
        for c in range(blocks):
            rows = pl.ds(j, SEGMENTS, stride=span)
            d = decay.at[c][rows, :]
            v = drive.at[c][rows, :]
            h = d * states[c] + v
            p = prods[c] * d
            drive.at[c][rows, :] = h
            decay.at[c][rows, :] = p
            new_h.append(h)
            new_p.append(p)
        return tuple(new_p), tuple(new_h)

    ones = tuple(jnp.ones((SEGMENTS, LANES), jnp.float32) for _ in range(blocks))
    zeros = tuple(jnp.zeros((SEGMENTS, LANES), jnp.float32) for _ in range(blocks))
    prods, states = lax.fori_loop(0, span, step, (ones, zeros))

    for c in range(blocks):
        p = jnp.ones((1, LANES), jnp.float32)
        h = jnp.zeros((1, LANES), jnp.float32)
        for s in range(SEGMENTS):
            seg_p[c, pl.ds(s, 1), :] = p
            seg_h[c, pl.ds(s, 1), :] = h
            h = prods[c][s : s + 1] * h + states[c][s : s + 1]
            p = p * prods[c][s : s + 1]
        mine[pl.ds(c, 1), :] = p
        mine[pl.ds(blocks + c, 1), :] = h

    def message(k):
        return pltpu.make_async_remote_copy(
            src_ref=mine,
            dst_ref=slots.at[k],
            send_sem=send_sems.at[k],
            recv_sem=recv_sems.at[k],
            device_id={"sp": lax.rem(me + k, n)},
            device_id_type=MESH,
        )

    def send(k, carry):
        message(k).start()
        return carry

    lax.fori_loop(1, n, send, 0)

    def one_gelu(c, carry):
        cols = pl.ds(pl.multiple_of(c * LANES, LANES), LANES)
        padded_gate = gate_ref[:, cols].astype(jnp.float32)
        out_f32 = jax.nn.gelu(padded_gate)
        seg = out_f32
        drive[c] = drive[c] * seg
        decay[c] = decay[c] * seg
        for s in range(SEGMENTS):
            rows = pl.ds(s * span, span)
            drive[c, rows, :] = drive[c, rows, :] + (
                decay[c, rows, :] * seg_h[c, pl.ds(s, 1), :]
            )
        return carry

    lax.fori_loop(0, blocks, one_gelu, 0)

    def receive(k, carry):
        message(k).wait()
        return carry

    lax.fori_loop(1, n, receive, 0)

    def compose(i, state):
        k = me - i
        part = slots[k]
        return part[:blocks] * state + part[blocks:]

    carried = lax.fori_loop(0, me, compose, jnp.zeros((blocks, LANES), jnp.float32))

    for c in range(blocks):
        for s in range(SEGMENTS):
            rows = pl.ds(s * span, span)
            entry = seg_p[c, pl.ds(s, 1), :] * carried[c : c + 1]
            out_ref[rows, pl.ds(c * LANES, LANES)] = (
                drive[c, rows, :] + decay[c, rows, :] * entry
            ).astype(jnp.bfloat16)


def diagonal(blocks, width):
    count, bw, _ = blocks.shape
    per = LANES // bw
    grouped = blocks.reshape(count // per, per, bw, bw)
    rows = []
    for i in range(per):
        rows.append(
            jnp.concatenate(
                [grouped[:, i] if i == j else jnp.zeros_like(grouped[:, i]) for j in range(per)],
                axis=-1,
            )
        )
    return jnp.concatenate(rows, axis=-2)


def mix(x_branch, gate_branch, conv_w, gate_a_w, gate_x_w, decay_rate, decay_extra):
    length, width = x_branch.shape
    n = lax.axis_size("sp")
    blocks = width // LANES
    vmem = pl.BlockSpec(memory_space=pltpu.VMEM)
    return pl.pallas_call(
        functools.partial(mixer_kernel, n, conv_w.shape[0]),
        out_shape=jax.ShapeDtypeStruct((length, width), jnp.bfloat16),
        in_specs=[vmem] * 7,
        out_specs=vmem,
        scratch_shapes=[
            pltpu.VMEM((HALO, width), jnp.bfloat16),
            pltpu.VMEM((length + 8, LANES), jnp.float32),
            pltpu.VMEM((blocks, length, LANES), jnp.float32),
            pltpu.VMEM((blocks, length, LANES), jnp.float32),
            pltpu.VMEM((blocks, SEGMENTS, LANES), jnp.float32),
            pltpu.VMEM((blocks, SEGMENTS, LANES), jnp.float32),
            pltpu.VMEM((2 * blocks, LANES), jnp.float32),
            pltpu.VMEM((n, 2 * blocks, LANES), jnp.float32),
            pltpu.SemaphoreType.DMA,
            pltpu.SemaphoreType.DMA,
            pltpu.SemaphoreType.DMA((n,)),
            pltpu.SemaphoreType.DMA((n,)),
        ],
        compiler_params=pltpu.CompilerParams(
            collective_id=0, has_side_effects=True, vmem_limit_bytes=24 * 1024 * 1024
        ),
        cost_estimate=pl.CostEstimate(
            flops=40_000 * length * width // 1024, bytes_accessed=12 * length * width, transcendentals=0
        ),
        name="mixer",
    )(
        x_branch,
        gate_branch,
        conv_w,
        diagonal(gate_a_w, width),
        diagonal(gate_x_w, width),
        decay_rate[None, :],
        decay_extra,
    )


def rms_scale(values, gains):
    return values * lax.rsqrt(jnp.mean(values * values, axis=-1, keepdims=True) + NORM_EPS) * gains


def shift(value, axis, steps):
    count = lax.axis_size(axis)
    return lax.ppermute(value, axis, [(i, (i + steps) % count) for i in range(count)])


def shards(
    resid,
    x_branch,
    gate_branch,
    conv_w,
    gate_a_w,
    gate_x_w,
    decay_rate,
    decay_extra,
    w_proj,
    mix_gain,
    pre_gain,
    w_gate,
    w_up,
    w_down,
    out_gain,
):
    n = lax.axis_size("sp")
    tp = lax.axis_size("tp")
    sp_at = lax.axis_index("sp")
    tp_at = lax.axis_index("tp")
    line = 4
    plane = n // line
    line_at = sp_at // plane
    plane_at = sp_at % plane
    ring = [0, 1, 3, 2] if plane == 4 else list(range(plane))
    ring_of = [ring.index(p) for p in range(plane)]

    def along_line(value, steps):
        pairs = [
            (z * plane + p, (z + steps) * plane + p)
            for z in range(line)
            for p in range(plane)
            if 0 <= z + steps < line
        ]
        return lax.ppermute(value, "sp", pairs)

    def round_line(value, steps):
        pairs = [
            (z * plane + p, ((z + steps) % line) * plane + p)
            for z in range(line)
            for p in range(plane)
        ]
        return lax.ppermute(value, "sp", pairs)

    def round_plane(value, steps):
        pairs = [
            (z * plane + ring[i], z * plane + ring[(i + steps) % plane])
            for z in range(line)
            for i in range(plane)
        ]
        return lax.ppermute(value, "sp", pairs)

    rows, units = w_gate.shape
    part = units // line
    packed = jnp.stack(
        [
            jnp.stack([w[:, z * part : (z + 1) * part] for z in range(line)])
            for w in (w_gate, w_up)
        ]
        + [w_down.reshape(line, part, rows).transpose(0, 2, 1)],
        axis=1,
    )
    own = lax.dynamic_index_in_dim(packed, line_at, 0, True).transpose(1, 0, 2, 3)
    stack = jnp.zeros((3, line, rows, part), packed.dtype)
    stack = lax.dynamic_update_slice_in_dim(stack, own, line_at, 1)
    arrived = []
    for s in range(1, line):
        piece = lax.dynamic_index_in_dim(packed, (line_at + s) % line, 0, True)
        arrived.append((s, round_line(piece.transpose(1, 0, 2, 3), s)))
    for s, piece in arrived:
        stack = lax.dynamic_update_slice_in_dim(stack, piece, (line_at - s) % line, 1)
    from_ring = {0: [stack]}
    ahead = behind = stack
    for k in range(1, plane // 2):
        ahead = round_plane(ahead, -1)
        behind = round_plane(behind, 1)
        from_ring[k] = [ahead]
        from_ring[plane - k] = [behind]
    low = round_plane(ahead[:, : line // 2], -1)
    high = round_plane(behind[:, line // 2 :], 1)
    from_ring[plane // 2] = [low, high]
    ring_at = jnp.asarray(ring_of)[plane_at]

    order = jnp.asarray(ring)[(ring_at + jnp.arange(plane)) % plane]
    back = (jnp.asarray(ring_of) - ring_at) % plane

    mixer = mix(x_branch, gate_branch, conv_w, gate_a_w, gate_x_w, decay_rate, decay_extra)
    length = mixer.shape[0]
    share = length // tp
    width = w_proj.shape[1]
    partial = jnp.dot(mixer, w_proj, preferred_element_type=jnp.float32).astype(jnp.bfloat16)

    def share_of(value, place):
        return lax.dynamic_slice_in_dim(value, place * share, share, 0)

    mixed = share_of(partial, tp_at).astype(jnp.float32)
    for i in range(1, tp):
        got = shift(share_of(partial, (tp_at + i) % tp), "tp", i)
        mixed = mixed + got.astype(jnp.float32)
    stream = share_of(resid, tp_at).astype(jnp.float32) + rms_scale(mixed, mix_gain)
    normed = rms_scale(stream, pre_gain).astype(jnp.bfloat16)

    cut = normed.reshape(share, line, plane, rows)
    mine = jnp.stack(
        [lax.dynamic_index_in_dim(cut, order[j], 2, False) for j in range(plane)], axis=1
    ).reshape(share, width)

    up = down = mine
    ups, downs = [], []
    for k in range(1, line):
        up = along_line(up, 1)
        down = along_line(down, -1)
        ups.append(up)
        downs.append(down)
    slots = [mine]
    for k in range(1, line):
        slots.append(jnp.where(line_at >= k, ups[k - 1], downs[line - k - 1]))

    pieces = []
    at = 0
    for j in range(plane):
        for piece in from_ring[j]:
            size = piece.shape[1] * rows
            pieces.append((at, size, piece.reshape(3, size, part)))
            at += size
    down_t = jnp.concatenate([piece[2] for _, _, piece in pieces], axis=0)

    def feed_forward(chosen):
        own_rows = jnp.concatenate([slots[k] for k in chosen], axis=0)
        parts = [own_rows] + [shift(own_rows, "tp", -i) for i in range(1, tp)]
        tokens = jnp.concatenate(parts, axis=0)
        gate = upward = None
        for start, size, piece in pieces:
            block = tokens[:, start : start + size]
            g = jnp.dot(block, piece[0], preferred_element_type=jnp.float32)
            u = jnp.dot(block, piece[1], preferred_element_type=jnp.float32)
            gate = g if gate is None else gate + g
            upward = u if upward is None else upward + u
        hidden = (jax.nn.silu(gate) * upward).astype(jnp.bfloat16)
        out = lax.dot_general(
            hidden, down_t, (((1,), (1,)), ((), ())), preferred_element_type=jnp.float32
        ).astype(jnp.bfloat16)
        out = out.reshape(tp, len(chosen) * share, width)
        total = out[0].astype(jnp.float32)
        for i in range(1, tp):
            total = total + shift(out[i], "tp", i).astype(jnp.float32)
        return {k: total[a * share : (a + 1) * share] for a, k in enumerate(chosen)}

    sums = {}
    for chosen in ([1, 3], [2, 0]) if line == 4 else ([k for k in range(line)],):
        sums.update(feed_forward(chosen))

    up_sum = down_sum = None
    for k in range(line - 1, 0, -1):
        to_up, to_down = sums[line - k], sums[k]
        if up_sum is not None:
            to_up = to_up + up_sum.astype(jnp.float32)
            to_down = to_down + down_sum.astype(jnp.float32)
        up_sum = along_line(to_up.astype(jnp.bfloat16), 1)
        down_sum = along_line(to_down.astype(jnp.bfloat16), -1)
    ffn = sums[0] + up_sum.astype(jnp.float32) + down_sum.astype(jnp.float32)
    ffn = ffn.reshape(share, plane, line, rows)
    ffn = jnp.stack(
        [lax.dynamic_index_in_dim(ffn, back[p], 1, False) for p in range(plane)], axis=2
    ).reshape(share, width)
    return (stream + 0.5 * rms_scale(ffn, out_gain)).astype(jnp.bfloat16)


def solution(mesh):
    return jax.shard_map(
        shards,
        mesh=mesh,
        in_specs=(
            P("sp", None),
            P("sp", "tp"),
            P("sp", "tp"),
            P(None, "tp"),
            P("tp", None, None),
            P("tp", None, None),
            P("tp"),
            P("sp", "tp"),
            P("tp", None),
            P(),
            P(),
            P("sp", "tp"),
            P("sp", "tp"),
            P("tp", "sp"),
            P(),
        ),
        out_specs=P(("sp", "tp"), None),
        check_vma=False,
    )
```

```python
import functools

import jax
import jax.numpy as jnp
from jax import lax
from jax.experimental import pallas as pl
from jax.experimental.pallas import tpu as pltpu
from jax.sharding import PartitionSpec as P

LRU_SCALE = 8.0
NORM_EPS = 1e-06
LANES = 128
SEGMENTS = 8
HALO = 16
MESH = pl.DeviceIdType.MESH


def neg_expm1(u):
    near = 1.0 + u * (1.0 / 8.0)
    for k in range(7, 1, -1):
        near = 1.0 + (u * (1.0 / k)) * near
    return jnp.where(u > -0.35, -u * near, 1.0 - jnp.exp(u))


def mixer_kernel(
    n,
    taps,
    x_ref,
    gate_ref,
    conv_ref,
    ga_ref,
    gx_ref,
    rate_ref,
    extra_ref,
    out_ref,
    halo,
    padded,
    decay,
    drive,
    seg_p,
    seg_h,
    mine,
    slots,
    halo_send,
    halo_recv,
    send_sems,
    recv_sems,
):
    me = lax.axis_index("sp")
    length, width = x_ref.shape
    blocks = width // LANES
    span = length // SEGMENTS

    barrier = pltpu.get_barrier_semaphore()

    def greet(k, carry):
        pl.semaphore_signal(
            barrier, inc=1, device_id={"sp": lax.rem(me + k, n)}, device_id_type=MESH
        )
        return carry

    lax.fori_loop(1, n, greet, 0)
    pl.semaphore_wait(barrier, n - 1)

    tail = pltpu.make_async_remote_copy(
        src_ref=x_ref.at[pl.ds(length - HALO, HALO)],
        dst_ref=halo,
        send_sem=halo_send,
        recv_sem=halo_recv,
        device_id={"sp": lax.rem(me + 1, n)},
        device_id_type=MESH,
    )
    tail.start()
    tail.wait()

    first_place = (me > 0).astype(jnp.float32)

    def one_block(c, carry):
        cols = pl.ds(pl.multiple_of(c * LANES, LANES), LANES)
        padded[pl.ds(8, length), :] = x_ref[:, cols].astype(jnp.float32)
        padded[pl.ds(0, 8), :] = halo[pl.ds(HALO - 8, 8), cols].astype(jnp.float32) * first_place
        start = 8 - (taps - 1)
        conv = padded[pl.ds(start, length), :] * conv_ref[pl.ds(0, 1), cols]
        for tap in range(1, taps):
            conv = conv + padded[pl.ds(start + tap, length), :] * conv_ref[pl.ds(tap, 1), cols]
        conv_out = conv.astype(jnp.bfloat16)
        recur = jax.nn.sigmoid(
            jnp.dot(conv_out, ga_ref[c], preferred_element_type=jnp.float32)
        )
        inject = jax.nn.sigmoid(
            jnp.dot(conv_out, gx_ref[c], preferred_element_type=jnp.float32)
        )
        log_decay = -LRU_SCALE * recur * rate_ref[pl.ds(0, 1), cols] + extra_ref[:, cols]
        decay[c] = jnp.exp(log_decay)
        room = neg_expm1(2.0 * log_decay)
        root = jnp.where(room > 0.0, jnp.sqrt(jnp.maximum(room, 1e-37)), 0.0)
        drive[c] = root * inject * conv_out.astype(jnp.float32)
        return carry

    lax.fori_loop(0, blocks, one_block, 0)

    def step(j, carry):
        prods, states = carry
        new_p, new_h = [], []
        for c in range(blocks):
            rows = pl.ds(j, SEGMENTS, stride=span)
            d = decay.at[c][rows, :]
            v = drive.at[c][rows, :]
            h = d * states[c] + v
            p = prods[c] * d
            drive.at[c][rows, :] = h
            decay.at[c][rows, :] = p
            new_h.append(h)
            new_p.append(p)
        return tuple(new_p), tuple(new_h)

    ones = tuple(jnp.ones((SEGMENTS, LANES), jnp.float32) for _ in range(blocks))
    zeros = tuple(jnp.zeros((SEGMENTS, LANES), jnp.float32) for _ in range(blocks))
    prods, states = lax.fori_loop(0, span, step, (ones, zeros))

    for c in range(blocks):
        p = jnp.ones((1, LANES), jnp.float32)
        h = jnp.zeros((1, LANES), jnp.float32)
        for s in range(SEGMENTS):
            seg_p[c, pl.ds(s, 1), :] = p
            seg_h[c, pl.ds(s, 1), :] = h
            h = prods[c][s : s + 1] * h + states[c][s : s + 1]
            p = p * prods[c][s : s + 1]
        mine[pl.ds(c, 1), :] = p
        mine[pl.ds(blocks + c, 1), :] = h

    def message(k):
        return pltpu.make_async_remote_copy(
            src_ref=mine,
            dst_ref=slots.at[k],
            send_sem=send_sems.at[k],
            recv_sem=recv_sems.at[k],
            device_id={"sp": lax.rem(me + k, n)},
            device_id_type=MESH,
        )

    def send(k, carry):
        message(k).start()
        return carry

    lax.fori_loop(1, n, send, 0)

    def one_gelu(c, carry):
        cols = pl.ds(pl.multiple_of(c * LANES, LANES), LANES)
        padded_gate = gate_ref[:, cols].astype(jnp.float32)
        out_f32 = jax.nn.gelu(padded_gate)
        seg = out_f32
        drive[c] = drive[c] * seg
        decay[c] = decay[c] * seg
        for s in range(SEGMENTS):
            rows = pl.ds(s * span, span)
            drive[c, rows, :] = drive[c, rows, :] + (
                decay[c, rows, :] * seg_h[c, pl.ds(s, 1), :]
            )
        return carry

    lax.fori_loop(0, blocks, one_gelu, 0)

    def receive(k, carry):
        message(k).wait()
        return carry

    lax.fori_loop(1, n, receive, 0)

    def compose(i, state):
        k = me - i
        part = slots[k]
        return part[:blocks] * state + part[blocks:]

    carried = lax.fori_loop(0, me, compose, jnp.zeros((blocks, LANES), jnp.float32))

    for c in range(blocks):
        for s in range(SEGMENTS):
            rows = pl.ds(s * span, span)
            entry = seg_p[c, pl.ds(s, 1), :] * carried[c : c + 1]
            out_ref[rows, pl.ds(c * LANES, LANES)] = (
                drive[c, rows, :] + decay[c, rows, :] * entry
            ).astype(jnp.bfloat16)


def diagonal(blocks):
    count, bw, _ = blocks.shape
    per = LANES // bw
    grouped = blocks.reshape(count // per, per, bw, bw)
    rows = []
    for i in range(per):
        rows.append(
            jnp.concatenate(
                [grouped[:, i] if i == j else jnp.zeros_like(grouped[:, i]) for j in range(per)],
                axis=-1,
            )
        )
    return jnp.concatenate(rows, axis=-2)


def mix(x_branch, gate_branch, conv_w, gate_a_w, gate_x_w, decay_rate, decay_extra):
    length, width = x_branch.shape
    n = lax.axis_size("sp")
    blocks = width // LANES
    vmem = pl.BlockSpec(memory_space=pltpu.VMEM)
    return pl.pallas_call(
        functools.partial(mixer_kernel, n, conv_w.shape[0]),
        out_shape=jax.ShapeDtypeStruct((length, width), jnp.bfloat16),
        in_specs=[vmem] * 7,
        out_specs=vmem,
        scratch_shapes=[
            pltpu.VMEM((HALO, width), jnp.bfloat16),
            pltpu.VMEM((length + 8, LANES), jnp.float32),
            pltpu.VMEM((blocks, length, LANES), jnp.float32),
            pltpu.VMEM((blocks, length, LANES), jnp.float32),
            pltpu.VMEM((blocks, SEGMENTS, LANES), jnp.float32),
            pltpu.VMEM((blocks, SEGMENTS, LANES), jnp.float32),
            pltpu.VMEM((2 * blocks, LANES), jnp.float32),
            pltpu.VMEM((n, 2 * blocks, LANES), jnp.float32),
            pltpu.SemaphoreType.DMA,
            pltpu.SemaphoreType.DMA,
            pltpu.SemaphoreType.DMA((n,)),
            pltpu.SemaphoreType.DMA((n,)),
        ],
        compiler_params=pltpu.CompilerParams(
            collective_id=0, has_side_effects=True, vmem_limit_bytes=24 * 1024 * 1024
        ),
        cost_estimate=pl.CostEstimate(
            flops=40_000 * length * width // 1024, bytes_accessed=12 * length * width, transcendentals=0
        ),
        name="mixer",
    )(
        x_branch,
        gate_branch,
        conv_w,
        diagonal(gate_a_w),
        diagonal(gate_x_w),
        decay_rate[None, :],
        decay_extra,
    )


VMEM = pl.BlockSpec(memory_space=pltpu.VMEM)


def lanes_at(block):
    return pl.ds(pl.multiple_of(block * LANES, LANES), LANES)


def pack_kernel(line, plane, gate_ref, up_ref, down_ref, *out_refs):
    part = gate_ref.shape[1] // line
    line_at = lax.axis_index("sp") // plane
    for z in range(line):
        units = pl.ds(z * part, part)
        flat = down_ref[units, :].astype(jnp.float32).T.astype(jnp.bfloat16)
        for s in range(line):

            @pl.when(lax.rem(line_at + s, line) == z)
            def _():
                out_refs[s][0, 0] = gate_ref[:, units]
                out_refs[s][1, 0] = up_ref[:, units]
                out_refs[s][2, 0] = flat


def pack(line, plane, w_gate, w_up, w_down):
    rows, units = w_gate.shape
    shape = jax.ShapeDtypeStruct((3, 1, rows, units // line), w_gate.dtype)
    return pl.pallas_call(
        functools.partial(pack_kernel, line, plane),
        out_shape=[shape] * line,
        in_specs=[VMEM] * 3,
        out_specs=[VMEM] * line,
        compiler_params=pltpu.CompilerParams(vmem_limit_bytes=24 * 1024 * 1024),
        name="pack",
    )(w_gate, w_up, w_down)


def ring_slot(ring, places, offset):
    plane = len(ring)
    here = lax.rem(lax.axis_index("sp"), plane)
    out = here * 0
    for p in range(plane):
        out = out + (here == p).astype(jnp.int32) * places(p, offset)
    return out


def enter_kernel(line, ring, count, *refs):
    parts, (resid_ref, mix_ref, pre_ref, stream_ref, mine_ref) = refs[:count], refs[count:]
    plane = len(ring)
    mixed = parts[0][...].astype(jnp.float32)
    for other in parts[1:]:
        mixed = mixed + other[...].astype(jnp.float32)
    stream = resid_ref[...].astype(jnp.float32) + rms_scale(mixed, mix_ref[...])
    stream_ref[...] = stream
    normed = rms_scale(stream, pre_ref[...]).astype(jnp.bfloat16)
    for p in range(plane):
        offset = ring_slot(ring, lambda q, p: (ring.index(p) - ring.index(q)) % plane, p)
        for z in range(line):
            at = (z * plane + p) * LANES
            mine_ref[:, lanes_at(offset * line + z)] = normed[:, at : at + LANES]


def enter(line, ring, parts, resid, mix_gain, pre_gain):
    share, width = resid.shape
    return pl.pallas_call(
        functools.partial(enter_kernel, line, ring, len(parts)),
        out_shape=[
            jax.ShapeDtypeStruct((share, width), jnp.float32),
            jax.ShapeDtypeStruct((share, width), jnp.bfloat16),
        ],
        in_specs=[VMEM] * (len(parts) + 3),
        out_specs=[VMEM] * 2,
        compiler_params=pltpu.CompilerParams(vmem_limit_bytes=24 * 1024 * 1024),
        name="enter",
    )(*parts, resid, mix_gain[None, :], pre_gain[None, :])


def leave_kernel(line, ring, own_ref, up_ref, down_ref, stream_ref, gain_ref, out_ref, ffn_ref):
    plane = len(ring)
    ffn = own_ref[...] + up_ref[...].astype(jnp.float32) + down_ref[...].astype(jnp.float32)
    ffn_ref[...] = ffn * (
        0.5 * lax.rsqrt(jnp.mean(ffn * ffn, axis=-1, keepdims=True) + NORM_EPS)
    )
    for p in range(plane):
        offset = ring_slot(ring, lambda q, p: (ring.index(p) - ring.index(q)) % plane, p)
        for z in range(line):
            cols = pl.ds((z * plane + p) * LANES, LANES)
            out_ref[:, cols] = (
                stream_ref[:, cols] + ffn_ref[:, lanes_at(offset * line + z)] * gain_ref[:, cols]
            ).astype(jnp.bfloat16)


def leave(line, ring, own, up_sum, down_sum, stream, out_gain):
    share, width = stream.shape
    return pl.pallas_call(
        functools.partial(leave_kernel, line, ring),
        out_shape=jax.ShapeDtypeStruct((share, width), jnp.bfloat16),
        in_specs=[VMEM] * 5,
        out_specs=VMEM,
        scratch_shapes=[pltpu.VMEM((share, width), jnp.float32)],
        compiler_params=pltpu.CompilerParams(vmem_limit_bytes=24 * 1024 * 1024),
        name="leave",
    )(own, up_sum, down_sum, stream, out_gain[None, :])


def hidden_kernel(tokens_ref, *refs):
    weights, out_ref = refs[:-1], refs[-1]
    gate = upward = None
    at = 0
    for w in weights:
        block = tokens_ref[:, at : at + w.shape[1]]
        g = jnp.dot(block, w[0], preferred_element_type=jnp.float32)
        u = jnp.dot(block, w[1], preferred_element_type=jnp.float32)
        gate = g if gate is None else gate + g
        upward = u if upward is None else upward + u
        at += w.shape[1]
    hidden = (jax.nn.silu(gate) * upward).astype(jnp.bfloat16)
    at = 0
    for w in weights:
        out_ref[:, at : at + w.shape[1]] = lax.dot_general(
            hidden, w[2], (((1,), (1,)), ((), ())), preferred_element_type=jnp.float32
        ).astype(jnp.bfloat16)
        at += w.shape[1]


def feed(tokens, pieces):
    rows, width = tokens.shape
    block = rows // 2
    part = pieces[0].shape[2]
    return pl.pallas_call(
        hidden_kernel,
        grid=(rows // block,),
        out_shape=jax.ShapeDtypeStruct((rows, width), jnp.bfloat16),
        in_specs=[pl.BlockSpec((block, width), lambda i: (i, 0))]
        + [pl.BlockSpec(p.shape, lambda i: (0, 0, 0)) for p in pieces],
        out_specs=pl.BlockSpec((block, width), lambda i: (i, 0)),
        compiler_params=pltpu.CompilerParams(vmem_limit_bytes=48 * 1024 * 1024),
        cost_estimate=pl.CostEstimate(
            flops=6 * rows * width * part, bytes_accessed=6 * width * part, transcendentals=0
        ),
        name="feed",
    )(tokens, *pieces)


def rms_scale(values, gains):
    return values * lax.rsqrt(jnp.mean(values * values, axis=-1, keepdims=True) + NORM_EPS) * gains


def shift(value, axis, steps):
    count = lax.axis_size(axis)
    return lax.ppermute(value, axis, [(i, (i + steps) % count) for i in range(count)])


def shards(
    resid,
    x_branch,
    gate_branch,
    conv_w,
    gate_a_w,
    gate_x_w,
    decay_rate,
    decay_extra,
    w_proj,
    mix_gain,
    pre_gain,
    w_gate,
    w_up,
    w_down,
    out_gain,
):
    n = lax.axis_size("sp")
    tp = lax.axis_size("tp")
    sp_at = lax.axis_index("sp")
    tp_at = lax.axis_index("tp")
    line = 4
    plane = n // line
    line_at = sp_at // plane
    plane_at = sp_at % plane
    ring = [0, 1, 3, 2] if plane == 4 else list(range(plane))
    ring_of = [ring.index(p) for p in range(plane)]

    def along_line(value, steps):
        pairs = [
            (z * plane + p, (z + steps) * plane + p)
            for z in range(line)
            for p in range(plane)
            if 0 <= z + steps < line
        ]
        return lax.ppermute(value, "sp", pairs)

    def round_line(value, steps):
        pairs = [
            (z * plane + p, ((z + steps) % line) * plane + p)
            for z in range(line)
            for p in range(plane)
        ]
        return lax.ppermute(value, "sp", pairs)

    def round_plane(value, steps):
        pairs = [
            (z * plane + ring[i], z * plane + ring[(i + steps) % plane])
            for z in range(line)
            for i in range(plane)
        ]
        return lax.ppermute(value, "sp", pairs)

    rows, units = w_gate.shape
    part = units // line
    aligned = rows % LANES == 0 and plane == 4
    if aligned:
        bundles = pack(line, plane, w_gate, w_up, w_down)
    else:
        packed = jnp.stack(
            [
                jnp.stack([w[:, z * part : (z + 1) * part] for z in range(line)])
                for w in (w_gate, w_up)
            ]
            + [w_down.reshape(line, part, rows).transpose(0, 2, 1)],
            axis=1,
        )
        bundles = [
            lax.dynamic_index_in_dim(packed, (line_at + s) % line, 0, True).transpose(1, 0, 2, 3)
            for s in range(line)
        ]
    stack = jnp.zeros((3, line, rows, part), w_gate.dtype)
    stack = lax.dynamic_update_slice_in_dim(stack, bundles[0], line_at, 1)
    arrived = []
    for s in range(1, line):
        arrived.append((s, round_line(bundles[s], s)))
    for s, piece in arrived:
        stack = lax.dynamic_update_slice_in_dim(stack, piece, (line_at - s) % line, 1)
    from_ring = {0: [stack]}
    ahead = behind = stack
    for k in range(1, plane // 2):
        ahead = round_plane(ahead, -1)
        behind = round_plane(behind, 1)
        from_ring[k] = [ahead]
        from_ring[plane - k] = [behind]
    low = round_plane(ahead[:, : line // 2], -1)
    high = round_plane(behind[:, line // 2 :], 1)
    from_ring[plane // 2] = [low, high]
    ring_at = jnp.asarray(ring_of)[plane_at]

    order = jnp.asarray(ring)[(ring_at + jnp.arange(plane)) % plane]
    back = (jnp.asarray(ring_of) - ring_at) % plane

    mixer = mix(x_branch, gate_branch, conv_w, gate_a_w, gate_x_w, decay_rate, decay_extra)
    length = mixer.shape[0]
    share = length // tp
    width = w_proj.shape[1]
    partial = jnp.dot(mixer, w_proj, preferred_element_type=jnp.float32).astype(jnp.bfloat16)

    def share_of(value, place):
        return lax.dynamic_slice_in_dim(value, place * share, share, 0)

    parts = [share_of(partial, tp_at)]
    for i in range(1, tp):
        parts.append(shift(share_of(partial, (tp_at + i) % tp), "tp", i))
    own_resid = share_of(resid, tp_at)
    if aligned:
        stream, mine = enter(line, ring, parts, own_resid, mix_gain, pre_gain)
    else:
        mixed = sum(part.astype(jnp.float32) for part in parts)
        stream = own_resid.astype(jnp.float32) + rms_scale(mixed, mix_gain)
        normed = rms_scale(stream, pre_gain).astype(jnp.bfloat16)
        cut = normed.reshape(share, line, plane, rows)
        mine = jnp.stack(
            [lax.dynamic_index_in_dim(cut, order[j], 2, False) for j in range(plane)], axis=1
        ).reshape(share, width)

    up = down = mine
    ups, downs = [], []
    for _ in range(1, line):
        up = along_line(up, 1)
        down = along_line(down, -1)
        ups.append(up)
        downs.append(down)
    slots = [mine]
    for k in range(1, line):
        slots.append(jnp.where(line_at >= k, ups[k - 1], downs[line - k - 1]))

    pieces = []
    for j in range(plane):
        for piece in from_ring[j]:
            pieces.append(piece.reshape(3, piece.shape[1] * rows, part))

    def feed_forward(chosen):
        own_rows = jnp.concatenate([slots[k] for k in chosen], axis=0)
        tokens = [own_rows] + [shift(own_rows, "tp", -i) for i in range(1, tp)]
        out = feed(jnp.concatenate(tokens, axis=0), pieces)
        out = out.reshape(tp, len(chosen) * share, width)
        total = out[0].astype(jnp.float32)
        for i in range(1, tp):
            total = total + shift(out[i], "tp", i).astype(jnp.float32)
        return {k: total[a * share : (a + 1) * share] for a, k in enumerate(chosen)}

    sums = {}
    for chosen in ([2, 0], [1, 3]) if line == 4 else ([k for k in range(line)],):
        sums.update(feed_forward(chosen))

    up_sum = down_sum = None
    for k in range(line - 1, 0, -1):
        to_up, to_down = sums[line - k], sums[k]
        if up_sum is not None:
            to_up = to_up + up_sum.astype(jnp.float32)
            to_down = to_down + down_sum.astype(jnp.float32)
        up_sum = along_line(to_up.astype(jnp.bfloat16), 1)
        down_sum = along_line(to_down.astype(jnp.bfloat16), -1)
    if aligned:
        return leave(line, ring, sums[0], up_sum, down_sum, stream, out_gain)
    ffn = sums[0] + up_sum.astype(jnp.float32) + down_sum.astype(jnp.float32)
    ffn = ffn.reshape(share, plane, line, rows)
    ffn = jnp.stack(
        [lax.dynamic_index_in_dim(ffn, back[p], 1, False) for p in range(plane)], axis=2
    ).reshape(share, width)
    return (stream + 0.5 * rms_scale(ffn, out_gain)).astype(jnp.bfloat16)


def solution(mesh):
    return jax.shard_map(
        shards,
        mesh=mesh,
        in_specs=(
            P("sp", None),
            P("sp", "tp"),
            P("sp", "tp"),
            P(None, "tp"),
            P("tp", None, None),
            P("tp", None, None),
            P("tp"),
            P("sp", "tp"),
            P("tp", None),
            P(),
            P(),
            P("sp", "tp"),
            P("sp", "tp"),
            P("tp", "sp"),
            P(),
        ),
        out_specs=P(("sp", "tp"), None),
        check_vma=False,
    )
```

```python
import functools

import jax
import jax.numpy as jnp
from jax import lax
from jax.experimental import pallas as pl
from jax.experimental.pallas import tpu as pltpu
from jax.sharding import PartitionSpec as P

LRU_SCALE = 8.0
NORM_EPS = 1e-06
LANES = 128
SEGMENTS = 8
HALO = 16
MESH = pl.DeviceIdType.MESH


def neg_expm1(u):
    near = 1.0 + u * (1.0 / 8.0)
    for k in range(7, 1, -1):
        near = 1.0 + (u * (1.0 / k)) * near
    return jnp.where(u > -0.35, -u * near, 1.0 - jnp.exp(u))


def mixer_kernel(
    n,
    taps,
    x_ref,
    gate_ref,
    conv_ref,
    ga_ref,
    gx_ref,
    rate_ref,
    extra_ref,
    out_ref,
    halo,
    padded,
    decay,
    drive,
    seg_p,
    seg_h,
    mine,
    slots,
    halo_send,
    halo_recv,
    send_sems,
    recv_sems,
):
    me = lax.axis_index("sp")
    length, width = x_ref.shape
    blocks = width // LANES
    span = length // SEGMENTS

    barrier = pltpu.get_barrier_semaphore()

    def greet(k, carry):
        pl.semaphore_signal(
            barrier, inc=1, device_id={"sp": lax.rem(me + k, n)}, device_id_type=MESH
        )
        return carry

    lax.fori_loop(1, n, greet, 0)
    pl.semaphore_wait(barrier, n - 1)

    tail = pltpu.make_async_remote_copy(
        src_ref=x_ref.at[pl.ds(length - HALO, HALO)],
        dst_ref=halo,
        send_sem=halo_send,
        recv_sem=halo_recv,
        device_id={"sp": lax.rem(me + 1, n)},
        device_id_type=MESH,
    )
    tail.start()
    tail.wait()

    first_place = (me > 0).astype(jnp.float32)

    def one_block(c, carry):
        cols = pl.ds(pl.multiple_of(c * LANES, LANES), LANES)
        padded[pl.ds(8, length), :] = x_ref[:, cols].astype(jnp.float32)
        padded[pl.ds(0, 8), :] = halo[pl.ds(HALO - 8, 8), cols].astype(jnp.float32) * first_place
        start = 8 - (taps - 1)
        conv = padded[pl.ds(start, length), :] * conv_ref[pl.ds(0, 1), cols]
        for tap in range(1, taps):
            conv = conv + padded[pl.ds(start + tap, length), :] * conv_ref[pl.ds(tap, 1), cols]
        conv_out = conv.astype(jnp.bfloat16)
        recur = jax.nn.sigmoid(
            jnp.dot(conv_out, ga_ref[c], preferred_element_type=jnp.float32)
        )
        inject = jax.nn.sigmoid(
            jnp.dot(conv_out, gx_ref[c], preferred_element_type=jnp.float32)
        )
        log_decay = -LRU_SCALE * recur * rate_ref[pl.ds(0, 1), cols] + extra_ref[:, cols]
        decay[c] = jnp.exp(log_decay)
        room = neg_expm1(2.0 * log_decay)
        root = jnp.where(room > 0.0, jnp.sqrt(jnp.maximum(room, 1e-37)), 0.0)
        drive[c] = root * inject * conv_out.astype(jnp.float32)
        return carry

    lax.fori_loop(0, blocks, one_block, 0)

    def step(j, carry):
        prods, states = carry
        new_p, new_h = [], []
        for c in range(blocks):
            rows = pl.ds(j, SEGMENTS, stride=span)
            d = decay.at[c][rows, :]
            v = drive.at[c][rows, :]
            h = d * states[c] + v
            p = prods[c] * d
            drive.at[c][rows, :] = h
            decay.at[c][rows, :] = p
            new_h.append(h)
            new_p.append(p)
        return tuple(new_p), tuple(new_h)

    ones = tuple(jnp.ones((SEGMENTS, LANES), jnp.float32) for _ in range(blocks))
    zeros = tuple(jnp.zeros((SEGMENTS, LANES), jnp.float32) for _ in range(blocks))
    prods, states = lax.fori_loop(0, span, step, (ones, zeros))

    for c in range(blocks):
        p = jnp.ones((1, LANES), jnp.float32)
        h = jnp.zeros((1, LANES), jnp.float32)
        for s in range(SEGMENTS):
            seg_p[c, pl.ds(s, 1), :] = p
            seg_h[c, pl.ds(s, 1), :] = h
            h = prods[c][s : s + 1] * h + states[c][s : s + 1]
            p = p * prods[c][s : s + 1]
        mine[pl.ds(c, 1), :] = p
        mine[pl.ds(blocks + c, 1), :] = h

    def message(k):
        return pltpu.make_async_remote_copy(
            src_ref=mine,
            dst_ref=slots.at[k],
            send_sem=send_sems.at[k],
            recv_sem=recv_sems.at[k],
            device_id={"sp": lax.rem(me + k, n)},
            device_id_type=MESH,
        )

    def send(k, carry):
        message(k).start()
        return carry

    lax.fori_loop(1, n, send, 0)

    def one_gelu(c, carry):
        cols = pl.ds(pl.multiple_of(c * LANES, LANES), LANES)
        padded_gate = gate_ref[:, cols].astype(jnp.float32)
        out_f32 = jax.nn.gelu(padded_gate)
        seg = out_f32
        drive[c] = drive[c] * seg
        decay[c] = decay[c] * seg
        for s in range(SEGMENTS):
            rows = pl.ds(s * span, span)
            drive[c, rows, :] = drive[c, rows, :] + (
                decay[c, rows, :] * seg_h[c, pl.ds(s, 1), :]
            )
        return carry

    lax.fori_loop(0, blocks, one_gelu, 0)

    def receive(k, carry):
        message(k).wait()
        return carry

    lax.fori_loop(1, n, receive, 0)

    def compose(i, state):
        k = me - i
        part = slots[k]
        return part[:blocks] * state + part[blocks:]

    carried = lax.fori_loop(0, me, compose, jnp.zeros((blocks, LANES), jnp.float32))

    for c in range(blocks):
        for s in range(SEGMENTS):
            rows = pl.ds(s * span, span)
            entry = seg_p[c, pl.ds(s, 1), :] * carried[c : c + 1]
            out_ref[rows, pl.ds(c * LANES, LANES)] = (
                drive[c, rows, :] + decay[c, rows, :] * entry
            ).astype(jnp.bfloat16)


def diagonal(blocks):
    count, bw, _ = blocks.shape
    per = LANES // bw
    grouped = blocks.reshape(count // per, per, bw, bw)
    rows = []
    for i in range(per):
        rows.append(
            jnp.concatenate(
                [grouped[:, i] if i == j else jnp.zeros_like(grouped[:, i]) for j in range(per)],
                axis=-1,
            )
        )
    return jnp.concatenate(rows, axis=-2)


def mix(x_branch, gate_branch, conv_w, gate_a_w, gate_x_w, decay_rate, decay_extra):
    length, width = x_branch.shape
    n = lax.axis_size("sp")
    blocks = width // LANES
    vmem = pl.BlockSpec(memory_space=pltpu.VMEM)
    return pl.pallas_call(
        functools.partial(mixer_kernel, n, conv_w.shape[0]),
        out_shape=jax.ShapeDtypeStruct((length, width), jnp.bfloat16),
        in_specs=[vmem] * 7,
        out_specs=vmem,
        scratch_shapes=[
            pltpu.VMEM((HALO, width), jnp.bfloat16),
            pltpu.VMEM((length + 8, LANES), jnp.float32),
            pltpu.VMEM((blocks, length, LANES), jnp.float32),
            pltpu.VMEM((blocks, length, LANES), jnp.float32),
            pltpu.VMEM((blocks, SEGMENTS, LANES), jnp.float32),
            pltpu.VMEM((blocks, SEGMENTS, LANES), jnp.float32),
            pltpu.VMEM((2 * blocks, LANES), jnp.float32),
            pltpu.VMEM((n, 2 * blocks, LANES), jnp.float32),
            pltpu.SemaphoreType.DMA,
            pltpu.SemaphoreType.DMA,
            pltpu.SemaphoreType.DMA((n,)),
            pltpu.SemaphoreType.DMA((n,)),
        ],
        compiler_params=pltpu.CompilerParams(
            collective_id=0, has_side_effects=True, vmem_limit_bytes=24 * 1024 * 1024
        ),
        cost_estimate=pl.CostEstimate(
            flops=40_000 * length * width // 1024, bytes_accessed=12 * length * width, transcendentals=0
        ),
        name="mixer",
    )(
        x_branch,
        gate_branch,
        conv_w,
        diagonal(gate_a_w),
        diagonal(gate_x_w),
        decay_rate[None, :],
        decay_extra,
    )


VMEM = pl.BlockSpec(memory_space=pltpu.VMEM)


def lanes_at(block):
    return pl.ds(pl.multiple_of(block * LANES, LANES), LANES)


def pack_kernel(line, plane, gate_ref, up_ref, down_ref, *out_refs):
    part = gate_ref.shape[1] // line
    line_at = lax.axis_index("sp") // plane
    for z in range(line):
        units = pl.ds(z * part, part)
        gate = gate_ref[:, units].astype(jnp.float32).T.astype(jnp.bfloat16)
        up = up_ref[:, units].astype(jnp.float32).T.astype(jnp.bfloat16)
        for s in range(line):

            @pl.when(lax.rem(line_at + s, line) == z)
            def _():
                out_refs[s][0] = gate
                out_refs[s][1] = up
                out_refs[s][2] = down_ref[units, :]


def pack(line, plane, w_gate, w_up, w_down):
    rows, units = w_gate.shape
    shape = jax.ShapeDtypeStruct((3, units // line, rows), w_gate.dtype)
    return pl.pallas_call(
        functools.partial(pack_kernel, line, plane),
        out_shape=[shape] * line,
        in_specs=[VMEM] * 3,
        out_specs=[VMEM] * line,
        compiler_params=pltpu.CompilerParams(vmem_limit_bytes=24 * 1024 * 1024),
        name="pack",
    )(w_gate, w_up, w_down)


def ring_slot(ring, places, offset):
    plane = len(ring)
    here = lax.rem(lax.axis_index("sp"), plane)
    out = here * 0
    for p in range(plane):
        out = out + (here == p).astype(jnp.int32) * places(p, offset)
    return out


def enter_kernel(line, ring, count, *refs):
    parts, (resid_ref, mix_ref, pre_ref, stream_ref, mine_ref) = refs[:count], refs[count:]
    plane = len(ring)
    mixed = parts[0][...].astype(jnp.float32)
    for other in parts[1:]:
        mixed = mixed + other[...].astype(jnp.float32)
    stream = resid_ref[...].astype(jnp.float32) + rms_scale(mixed, mix_ref[...])
    stream_ref[...] = stream
    normed = rms_scale(stream, pre_ref[...]).astype(jnp.bfloat16)
    for p in range(plane):
        offset = ring_slot(ring, lambda q, p: (ring.index(p) - ring.index(q)) % plane, p)
        for z in range(line):
            at = (z * plane + p) * LANES
            mine_ref[:, lanes_at(offset * line + z)] = normed[:, at : at + LANES]


def enter(line, ring, parts, resid, mix_gain, pre_gain):
    share, width = resid.shape
    return pl.pallas_call(
        functools.partial(enter_kernel, line, ring, len(parts)),
        out_shape=[
            jax.ShapeDtypeStruct((share, width), jnp.float32),
            jax.ShapeDtypeStruct((share, width), jnp.bfloat16),
        ],
        in_specs=[VMEM] * (len(parts) + 3),
        out_specs=[VMEM] * 2,
        compiler_params=pltpu.CompilerParams(vmem_limit_bytes=24 * 1024 * 1024),
        name="enter",
    )(*parts, resid, mix_gain[None, :], pre_gain[None, :])


def leave_kernel(line, ring, own_ref, up_ref, down_ref, stream_ref, gain_ref, out_ref, ffn_ref):
    plane = len(ring)
    ffn = own_ref[...] + up_ref[...].astype(jnp.float32) + down_ref[...].astype(jnp.float32)
    ffn_ref[...] = ffn * (
        0.5 * lax.rsqrt(jnp.mean(ffn * ffn, axis=-1, keepdims=True) + NORM_EPS)
    )
    for p in range(plane):
        offset = ring_slot(ring, lambda q, p: (ring.index(p) - ring.index(q)) % plane, p)
        for z in range(line):
            cols = pl.ds((z * plane + p) * LANES, LANES)
            out_ref[:, cols] = (
                stream_ref[:, cols] + ffn_ref[:, lanes_at(offset * line + z)] * gain_ref[:, cols]
            ).astype(jnp.bfloat16)


def leave(line, ring, own, up_sum, down_sum, stream, out_gain):
    share, width = stream.shape
    return pl.pallas_call(
        functools.partial(leave_kernel, line, ring),
        out_shape=jax.ShapeDtypeStruct((share, width), jnp.bfloat16),
        in_specs=[VMEM] * 5,
        out_specs=VMEM,
        scratch_shapes=[pltpu.VMEM((share, width), jnp.float32)],
        compiler_params=pltpu.CompilerParams(vmem_limit_bytes=24 * 1024 * 1024),
        name="leave",
    )(own, up_sum, down_sum, stream, out_gain[None, :])


def feed_kernel(count, *refs):
    tokens, weights, outs = refs[:count], refs[count:-count], refs[-count:]
    over_features = (((1,), (1,)), ((), ()))
    for token_ref, out_ref in zip(tokens, outs):
        gate = upward = None
        at = 0
        for w in weights:
            size = w.shape[2]
            block = token_ref[:, at : at + size]
            g = lax.dot_general(block, w[0], over_features, preferred_element_type=jnp.float32)
            u = lax.dot_general(block, w[1], over_features, preferred_element_type=jnp.float32)
            gate = g if gate is None else gate + g
            upward = u if upward is None else upward + u
            at += size
        hidden = (jax.nn.silu(gate) * upward).astype(jnp.bfloat16)
        at = 0
        for w in weights:
            size = w.shape[2]
            out_ref[:, at : at + size] = jnp.dot(
                hidden, w[2], preferred_element_type=jnp.float32
            ).astype(jnp.bfloat16)
            at += size


def feed(tokens, pieces):
    rows, width = tokens[0].shape
    count = len(tokens)
    part = pieces[0].shape[1]
    return pl.pallas_call(
        functools.partial(feed_kernel, count),
        out_shape=[jax.ShapeDtypeStruct((rows, width), jnp.bfloat16)] * count,
        in_specs=[VMEM] * (count + len(pieces)),
        out_specs=[VMEM] * count,
        compiler_params=pltpu.CompilerParams(vmem_limit_bytes=48 * 1024 * 1024),
        cost_estimate=pl.CostEstimate(
            flops=6 * count * rows * width * part,
            bytes_accessed=6 * width * part,
            transcendentals=0,
        ),
        name="feed",
    )(*tokens, *pieces)


def rms_scale(values, gains):
    return values * lax.rsqrt(jnp.mean(values * values, axis=-1, keepdims=True) + NORM_EPS) * gains


def shift(value, axis, steps):
    count = lax.axis_size(axis)
    return lax.ppermute(value, axis, [(i, (i + steps) % count) for i in range(count)])


def shards(
    resid,
    x_branch,
    gate_branch,
    conv_w,
    gate_a_w,
    gate_x_w,
    decay_rate,
    decay_extra,
    w_proj,
    mix_gain,
    pre_gain,
    w_gate,
    w_up,
    w_down,
    out_gain,
):
    n = lax.axis_size("sp")
    tp = lax.axis_size("tp")
    sp_at = lax.axis_index("sp")
    tp_at = lax.axis_index("tp")
    line = 4
    plane = n // line
    line_at = sp_at // plane
    plane_at = sp_at % plane
    ring = [0, 1, 3, 2] if plane == 4 else list(range(plane))
    ring_of = [ring.index(p) for p in range(plane)]

    def along_line(value, steps):
        pairs = [
            (z * plane + p, (z + steps) * plane + p)
            for z in range(line)
            for p in range(plane)
            if 0 <= z + steps < line
        ]
        return lax.ppermute(value, "sp", pairs)

    def round_line(value, steps):
        pairs = [
            (z * plane + p, ((z + steps) % line) * plane + p)
            for z in range(line)
            for p in range(plane)
        ]
        return lax.ppermute(value, "sp", pairs)

    def round_plane(value, steps):
        pairs = [
            (z * plane + ring[i], z * plane + ring[(i + steps) % plane])
            for z in range(line)
            for i in range(plane)
        ]
        return lax.ppermute(value, "sp", pairs)

    rows, units = w_gate.shape
    part = units // line
    aligned = rows % LANES == 0 and plane == 4
    if aligned:
        bundles = pack(line, plane, w_gate, w_up, w_down)
    else:
        packed = jnp.stack(
            [
                jnp.stack([w[:, z * part : (z + 1) * part].T for z in range(line)])
                for w in (w_gate, w_up)
            ]
            + [w_down.reshape(line, part, rows)],
            axis=1,
        )
        bundles = [
            lax.dynamic_index_in_dim(packed, (line_at + s) % line, 0, False) for s in range(line)
        ]
    stack = jnp.zeros((3, part, line * rows), w_gate.dtype)
    stack = lax.dynamic_update_slice_in_dim(stack, bundles[0], line_at * rows, 2)
    arrived = []
    for s in range(1, line):
        arrived.append((s, round_line(bundles[s], s)))
    for s, piece in arrived:
        stack = lax.dynamic_update_slice_in_dim(stack, piece, (line_at - s) % line * rows, 2)
    from_ring = {0: [stack]}
    ahead = behind = stack
    for k in range(1, plane // 2):
        ahead = round_plane(ahead, -1)
        behind = round_plane(behind, 1)
        from_ring[k] = [ahead]
        from_ring[plane - k] = [behind]
    middle = line // 2 * rows
    low = round_plane(ahead[:, :, :middle], -1)
    high = round_plane(behind[:, :, middle:], 1)
    from_ring[plane // 2] = [low, high]
    ring_at = jnp.asarray(ring_of)[plane_at]

    order = jnp.asarray(ring)[(ring_at + jnp.arange(plane)) % plane]
    back = (jnp.asarray(ring_of) - ring_at) % plane

    mixer = mix(x_branch, gate_branch, conv_w, gate_a_w, gate_x_w, decay_rate, decay_extra)
    length = mixer.shape[0]
    share = length // tp
    width = w_proj.shape[1]
    partial = jnp.dot(mixer, w_proj, preferred_element_type=jnp.float32).astype(jnp.bfloat16)

    def share_of(value, place):
        return lax.dynamic_slice_in_dim(value, place * share, share, 0)

    parts = [share_of(partial, tp_at)]
    for i in range(1, tp):
        parts.append(shift(share_of(partial, (tp_at + i) % tp), "tp", i))
    own_resid = share_of(resid, tp_at)
    if aligned:
        stream, mine = enter(line, ring, parts, own_resid, mix_gain, pre_gain)
    else:
        mixed = sum(part.astype(jnp.float32) for part in parts)
        stream = own_resid.astype(jnp.float32) + rms_scale(mixed, mix_gain)
        normed = rms_scale(stream, pre_gain).astype(jnp.bfloat16)
        cut = normed.reshape(share, line, plane, rows)
        mine = jnp.stack(
            [lax.dynamic_index_in_dim(cut, order[j], 2, False) for j in range(plane)], axis=1
        ).reshape(share, width)

    up = down = mine
    ups, downs = [], []
    for _ in range(1, line):
        up = along_line(up, 1)
        down = along_line(down, -1)
        ups.append(up)
        downs.append(down)
    slots = [mine]
    for k in range(1, line):
        slots.append(jnp.where(line_at >= k, ups[k - 1], downs[line - k - 1]))

    pieces = []
    for j in range(plane):
        for piece in from_ring[j]:
            pieces.append(piece)

    def feed_forward(chosen):
        own_rows = jnp.concatenate([slots[k] for k in chosen], axis=0)
        tokens = [own_rows] + [shift(own_rows, "tp", -i) for i in range(1, tp)]
        out = feed(tokens, pieces)
        total = out[0].astype(jnp.float32)
        for i in range(1, tp):
            total = total + shift(out[i], "tp", i).astype(jnp.float32)
        return {k: total[a * share : (a + 1) * share] for a, k in enumerate(chosen)}

    sums = {}
    for chosen in ([1, 3], [2, 0]):
        sums.update(feed_forward(chosen))

    up_sum = down_sum = None
    for k in range(line - 1, 0, -1):
        to_up, to_down = sums[line - k], sums[k]
        if up_sum is not None:
            to_up = to_up + up_sum.astype(jnp.float32)
            to_down = to_down + down_sum.astype(jnp.float32)
        up_sum = along_line(to_up.astype(jnp.bfloat16), 1)
        down_sum = along_line(to_down.astype(jnp.bfloat16), -1)
    if aligned:
        return leave(line, ring, sums[0], up_sum, down_sum, stream, out_gain)
    ffn = sums[0] + up_sum.astype(jnp.float32) + down_sum.astype(jnp.float32)
    ffn = ffn.reshape(share, plane, line, rows)
    ffn = jnp.stack(
        [lax.dynamic_index_in_dim(ffn, back[p], 1, False) for p in range(plane)], axis=2
    ).reshape(share, width)
    return (stream + 0.5 * rms_scale(ffn, out_gain)).astype(jnp.bfloat16)


def solution(mesh):
    return jax.shard_map(
        shards,
        mesh=mesh,
        in_specs=(
            P("sp", None),
            P("sp", "tp"),
            P("sp", "tp"),
            P(None, "tp"),
            P("tp", None, None),
            P("tp", None, None),
            P("tp"),
            P("sp", "tp"),
            P("tp", None),
            P(),
            P(),
            P("sp", "tp"),
            P("sp", "tp"),
            P("tp", "sp"),
            P(),
        ),
        out_specs=P(("sp", "tp"), None),
        check_vma=False,
    )
```
